32 devices in a mesh: grp: 2 (over y), ep: 4 (over z), tp: 4 (over x, core).
Axes of the slice: x: 2, y: 2, z: 4, core: 2. Of those that a mesh axis runs over, the one named last changes fastest.
Arguments:
- tokens: bfloat16 [2048, 2048], P(('grp', 'ep'), 'tp'), parts along dimension 0, may hold values from -6 to 6
- norm_gain: float32 [2048], replicated, may hold values from 0.1 to 1.9
- expert_ids: int32 [2048, 2], P(('grp', 'ep')), parts along dimension 0, may hold values from 0 to 3, all different within a row; in each aligned block of 256 rows (0 to 255, 256 to 511, ...) at most 192 rows name the same one
- gate_weights: float32 [2048, 2], P(('grp', 'ep')), parts along dimension 0, may hold values from 0.25 to 1
- w_gate: bfloat16 [4, 2048, 3072], P('ep', None, 'tp'), may hold values from -0.125 to 0.125
- w_up: bfloat16 [4, 2048, 3072], P('ep', None, 'tp'), may hold values from -0.125 to 0.125
- w_down: bfloat16 [4, 3072, 2048], P('ep', 'tp'), may hold values from -0.15625 to 0.15625
Outputs:
- mixed: bfloat16 [2048, 2048], P(('grp', 'ep'), 'tp'), parts along dimension 0
The draws below stay inside these ranges and needn't reach their ends.
There are 2 independent parts, one for each index of `grp`. The reference program is written for one: setup_inputs(seed, part) draws one part's arguments, and reference() takes and returns one part's arrays. A program takes and returns all parts, laid end to end along the dimension named above; an argument that names none is the same for every part. Nothing has to cross between parts.
Inputs may be any that keep to these rules, and one draw needn't show every extreme that they name: `expert_ids`: each token names 2 different experts. Within the 256 rows of one index of ep (aligned blocks) no expert is named more than 192 times, and in some blocks one expert is named exactly 192 times.
All inputs are finite; a program needn't handle non-finite values.
Results may differ from the reference program's by a relative error of at most 0.015.
Values may be sent and summed in bfloat16 or wider, within the bound.
No kernel may reach another device: no remote copies, remote signals or barrier semaphores. Data moves between devices by JAX's collectives and lax.ppermute only.
A program may use at most 64 MiB of HBM per device.

```python
import math
import jax
import jax.numpy as jnp
import numpy as np
from jax import lax

D = 2048
FF = 3072
TOP = 2
TOK_DEV = 256
EXPERTS = 4
CAP = 192
TOKENS = 1024
N_EP = 4
N_TP = 4


def with_spikes(result, stream_key, source, target, blocks, factor):
    def block_of(dim):
        return (jnp.arange(result.shape[dim]) // (result.shape[dim] // blocks)).reshape((-1,) + (1,) * (result.ndim - 1 - dim))

    one_side = jax.random.permutation(stream_key, blocks)[block_of(target)]
    other_side = (block_of(target) + blocks // 2) % blocks
    return jnp.where((block_of(source) == one_side) | (block_of(source) == other_side), factor * result, result)


def block_levels(own_key, extent, shards, least, top_value):
    def one(dim, parts):
        steps = jax.random.uniform(jax.random.fold_in(jax.random.fold_in(own_key, 6), dim), (parts,), jnp.float32, least / len(shards), top_value / len(shards))
        return jnp.repeat(jnp.exp(steps), extent[dim] // parts).reshape((-1,) + (1,) * (len(extent) - dim - 1))

    level = one(*shards[0])
    for cut in shards[1:]:
        level = level * one(*cut)
    return level


def deal_out(key, own, number, rows, amount, top, reach, slope):
    ranking = jax.random.permutation(key, amount)
    packed, ordinary = shares(amount, rows * top, reach, slope, True), shares(amount, rows * top, reach, slope, False)
    places = jnp.arange(amount)

    def named(lengths, turn):
        used = int((lengths > 0).sum())
        fixed = max(1, used // 4)
        passed = fixed + (places - fixed + turn * (used - fixed)) % max(1, amount - fixed)
        return jnp.zeros((amount,), jnp.int32).at[ranking[jnp.where(places < fixed, places, passed)]].set(jnp.asarray(lengths, jnp.int32))

    lengths = jnp.where(number % 4 == 0, named(packed, number // 4), named(ordinary, number - number // 4 - 1))
    mixed = jax.random.permutation(jax.random.fold_in(own, 3), amount)
    donor, receiver = mixed[0:amount // 2 * 2:2], mixed[1:amount // 2 * 2:2]
    slack = jnp.minimum(lengths[donor] - 1, reach - lengths[receiver]) // 2
    slack = jnp.where((donor == ranking[0]) | (receiver == ranking[0]) | (lengths[receiver] == 0), 0, jnp.maximum(slack, 0))
    passed = jax.random.randint(jax.random.fold_in(own, 4), (amount // 2,), 0, 1 << 20) % (slack + 1)
    lengths = lengths.at[donor].add(-passed).at[receiver].add(passed)
    members = jnp.searchsorted(jnp.cumsum(lengths), jnp.arange(rows * top), side="right").astype(jnp.int32)
    listing = members.reshape(top, rows).T
    listing = listing[jax.random.permutation(jax.random.fold_in(own, 1), rows)]
    turn = jax.random.randint(jax.random.fold_in(own, 2), (rows, 1), 0, top)
    return jnp.take_along_axis(listing, (jnp.arange(top)[None, :] + turn) % top, axis=1)


def shares(number_of, total, bound, skew, full):
    portions = [(1 << 20) // math.isqrt(rank ** skew) + 1 for rank in range(1, number_of + 1)]
    largest = bound if full else min(bound, max(-(-total // number_of), total * portions[0] // sum(portions)))
    least = 1 if total - largest >= number_of - 1 else 0
    given, spare = [largest] + [least] * (number_of - 1), total - largest - least * (number_of - 1)
    while spare > 0:
        free = [i for i in range(1, number_of) if given[i] < largest] or [i for i in range(1, number_of) if given[i] < bound]
        pool, budget = sum([portions[i] for i in free]), spare
        for i in free:
            extra = min(bound - given[i], max(1, budget * portions[i] // pool), spare)
            given[i] = given[i] + extra
            spare = spare - extra
    return np.array(given)


def gaussian(key, dims, spread, bound, split=(), kind=jnp.bfloat16):
    array = jax.random.normal(key, dims, jnp.float32) * spread
    if len(split) > 0:
        array = block_levels(key, dims, split, -0.22, 0.18) * array
    return jnp.clip(array, min=-bound, max=bound).astype(kind)


def heavy_noise(key, shape, spread, most, shards, heavy, kind=jnp.bfloat16):
    values = spread * jax.random.normal(key, shape, jnp.float32)
    if shards:
        values = values * block_levels(key, shape, shards, -0.22, 0.18)
    return jnp.clip(with_spikes(values, jax.random.fold_in(key, 3), *heavy), -most, most).astype(kind)


def setup_inputs(seed: int = 0, part: int = 0) -> dict:
    seeds = jax.random.split(jax.random.key(seed), 8)
    own_keys = jax.random.split(jax.random.fold_in(seeds[7], part), 8)
    tokens = gaussian(own_keys[0], (TOKENS, D), 1.0, 6.0, ((0, 4), (1, 4)))
    norm_gain = jnp.clip(1.0 + 0.18 * jax.random.normal(seeds[1], (D,), jnp.float32), 0.1, 1.9)
    expert_ids_keys = jax.random.split(jax.random.fold_in(own_keys[2], 1), TOKENS // TOK_DEV)
    expert_ids_turns = jax.random.permutation(jax.random.fold_in(own_keys[2], 3), TOKENS // TOK_DEV)
    expert_ids = jax.vmap(lambda own, number: deal_out(jax.random.fold_in(own_keys[2], 2), own, number, TOK_DEV, EXPERTS, TOP, CAP, 2))(expert_ids_keys, expert_ids_turns).reshape((TOKENS, TOP))
    gate_weights = jnp.clip(0.25 + 0.75 * jax.random.uniform(own_keys[3], (TOKENS, TOP), jnp.float32) ** block_levels(own_keys[3], (TOKENS, TOP), ((0, 4),), -0.2, 0.2), 0.25, 1.0)
    w_gate = gaussian(seeds[4], (EXPERTS, D, FF), D ** -0.5, 0.125, ((0, 4), (2, 4)))
    w_up = gaussian(seeds[5], (EXPERTS, D, FF), D ** -0.5, 0.125, ((0, 4), (2, 4)))
    w_down = heavy_noise(seeds[6], (EXPERTS, FF, D), FF ** -0.5, 0.15625, ((0, 4), (1, 4)), (1, 2, 4, 2.0))
    return dict(tokens=tokens, norm_gain=norm_gain, expert_ids=expert_ids, gate_weights=gate_weights, w_gate=w_gate, w_up=w_up, w_down=w_down)


epsilon = 1e-06

def reference(tokens, norm_gain, expert_ids, gate_weights, w_gate, w_up, w_down):
    tok_values = tokens.astype(jnp.float32)
    mean_square = lax.optimization_barrier(jnp.mean(tok_values * tok_values, axis=1, keepdims=True))
    normed = (tok_values * lax.rsqrt(mean_square + epsilon) * norm_gain.astype(jnp.float32)).astype(jnp.bfloat16)
    assign_count = TOK_DEV * TOP
    block_ids = expert_ids.reshape(N_EP, assign_count)
    onehot = (block_ids[:, :, None] == jnp.arange(EXPERTS, dtype=jnp.int32)[None, None, :]).astype(jnp.int32)
    earlier = jnp.cumsum(onehot, axis=1) - onehot
    slot_index = lax.optimization_barrier(jnp.sum(earlier * onehot, axis=2)).astype(jnp.int32)
    block_index = jnp.arange(N_EP, dtype=jnp.int32)[:, None]
    dest_index = ((block_ids * N_EP + block_index) * CAP + slot_index).astype(jnp.int32)
    owner_index = (block_index * TOK_DEV + jnp.arange(assign_count, dtype=jnp.int32)[None, :] // TOP).astype(jnp.int32)
    slot_token = jnp.full((EXPERTS * N_EP * CAP,), TOKENS, jnp.int32)
    slot_token = slot_token.at[dest_index.reshape(-1)].set(owner_index.reshape(-1))
    slot_token = slot_token.reshape(EXPERTS, N_EP * CAP)

    def run_expert(inputs):
        token_list, gate_matrix, up_matrix, down_matrix = inputs
        tok_rows = jnp.take(normed, token_list, axis=0, mode='fill', fill_value=0)
        gate_part = jnp.dot(tok_rows, gate_matrix, preferred_element_type=jnp.float32)
        up_part = jnp.dot(tok_rows, up_matrix, preferred_element_type=jnp.float32)
        hidden = (jax.nn.silu(gate_part) * up_part).astype(jnp.bfloat16)
        hidden_blocks = hidden.reshape(-1, N_TP, FF // N_TP).astype(jnp.float32)
        down_blocks = down_matrix.reshape(N_TP, FF // N_TP, D).astype(jnp.float32)
        partial_value = jnp.einsum('mtf,tfd->tmd', hidden_blocks, down_blocks).astype(jnp.bfloat16)
        partial_value = lax.optimization_barrier(partial_value)
        return lax.optimization_barrier(jnp.sum(partial_value.astype(jnp.float32), axis=0)).astype(jnp.bfloat16)
    expert_out = lax.map(run_expert, (slot_token, w_gate, w_up, w_down))
    picked = expert_out.reshape(-1, D)[dest_index.reshape(-1)].astype(jnp.float32)
    weighted = picked * gate_weights.reshape(-1)[:, None].astype(jnp.float32)
    return lax.optimization_barrier(jnp.sum(weighted.reshape(TOKENS, TOP, D), axis=1)).astype(jnp.bfloat16)
```

```python
import functools

import jax
import jax.numpy as jnp
from jax import lax
from jax.experimental import pallas as pl
from jax.experimental.pallas import tpu as pltpu
from jax.sharding import PartitionSpec as P

epsilon = 1e-06
VMEM = pltpu.MemorySpace.VMEM
MIB = 1 << 20


def is_power(number):
    return number & (number - 1) == 0


def exchange(array, axis, offset):
    size = lax.axis_size(axis)
    return lax.ppermute(array, axis, [(i, i ^ offset) for i in range(size)])


def call(kernel, outs, args, scratch=(), limit=16, flops=0, name=None):
    moved = sum(a.size * a.dtype.itemsize for a in (*args, *outs))
    return pl.pallas_call(
        kernel,
        out_shape=outs,
        in_specs=[pl.BlockSpec(memory_space=VMEM)] * len(args),
        out_specs=[pl.BlockSpec(memory_space=VMEM)] * len(outs),
        scratch_shapes=list(scratch),
        compiler_params=pltpu.CompilerParams(vmem_limit_bytes=limit * MIB),
        cost_estimate=pl.CostEstimate(flops=flops, bytes_accessed=moved, transcendentals=0),
        name=name,
    )(*args)


def match_rows(ids_ref, experts):
    top_count, tok_count = ids_ref.shape
    ids = ids_ref[...]
    named = []
    for expert in experts:
        hit = ids[0:1] == expert
        for k in range(1, top_count):
            hit = hit | (ids[k : k + 1] == expert)
        named.append(hit)
    ones = [jnp.where(hit, 1.0, 0.0) for hit in named]
    pad = -len(ones) % 8
    stacked = jnp.concatenate(ones + [jnp.zeros((pad, tok_count), jnp.float32)] * (pad > 0), axis=0)
    row = lax.broadcasted_iota(jnp.int32, (tok_count, tok_count), 0)
    col = lax.broadcasted_iota(jnp.int32, (tok_count, tok_count), 1)
    before = jnp.where(row < col, 1.0, 0.0).astype(jnp.bfloat16)
    places = jnp.dot(stacked.astype(jnp.bfloat16), before, preferred_element_type=jnp.float32)
    places = places.astype(jnp.int32)
    return named, [places[i : i + 1] for i in range(len(experts))]


def select_kernel(offsets, ids_ref, tok_ref, *out_refs):
    me = lax.axis_index("ep")
    named, places = match_rows(ids_ref, [me ^ s for s in offsets])
    tokens = tok_ref[...]
    for hit, place, out_ref in zip(named, places, out_refs):
        shape = (out_ref.shape[0], tokens.shape[0])
        slot = lax.broadcasted_iota(jnp.int32, shape, 0)
        pick = jnp.where((slot == place) & hit, 1.0, 0.0).astype(jnp.bfloat16)
        out_ref[...] = jnp.dot(pick, tokens, preferred_element_type=jnp.float32).astype(out_ref.dtype)


def combine_kernel(offsets, ids_ref, weight_ref, *refs):
    out_ref = refs[-1]
    me = lax.axis_index("ep")
    experts = [me ^ s for s in offsets]
    named, places = match_rows(ids_ref, experts)
    ids, weights = ids_ref[...], weight_ref[...]
    total = jnp.zeros(out_ref.shape, jnp.float32)
    for expert, hit, place, ref in zip(experts, named, places, refs[:-1]):
        weight = jnp.zeros(hit.shape, jnp.float32)
        for k in range(ids.shape[0]):
            weight = weight + jnp.where(ids[k : k + 1] == expert, weights[k : k + 1], 0.0)
        slot = lax.broadcasted_iota(jnp.int32, (ref.shape[0], ids.shape[1]), 0)
        spread = jnp.where((slot == place) & hit, weight, 0.0)
        high = spread.astype(jnp.bfloat16)
        low = (spread - high.astype(jnp.float32)).astype(jnp.bfloat16)
        rows = ref[...]
        for part in (high, low):
            total = total + lax.dot_general(
                part, rows, (((0,), (0,)), ((), ())), preferred_element_type=jnp.float32
            )
    out_ref[...] = total.astype(out_ref.dtype)


def expert_kernel(offsets, kept, sent, gain_ref, gate_ref, up_ref, down_ref, *refs):
    parts = refs[: len(offsets)]
    keep_ref, send_ref, normed, hidden = refs[len(offsets) :]
    me = lax.axis_index("tp")
    cols = parts[0].shape[1]
    width = cols * len(offsets)
    square_sum = None
    for ref in parts:
        values = ref[...].astype(jnp.float32)
        own = jnp.sum(values * values, axis=1, keepdims=True)
        square_sum = own if square_sum is None else square_sum + own
    scale = lax.rsqrt(square_sum / width + epsilon)
    for j, (offset, ref) in enumerate(zip(offsets, parts)):
        gain = gain_ref[me ^ offset]
        normed[j] = (ref[...].astype(jnp.float32) * scale * gain).astype(jnp.bfloat16)
    units = hidden.shape[1]
    tile = 256 if units % 256 == 0 else units

    def make_hidden(n, carry):
        span = pl.ds(pl.multiple_of(n * tile, tile), tile)
        gate = up = None
        for j, offset in enumerate(offsets):
            rows = pl.ds(pl.multiple_of((me ^ offset) * cols, cols), cols)
            values = normed[j]
            g = jnp.dot(values, gate_ref[0, rows, span], preferred_element_type=jnp.float32)
            u = jnp.dot(values, up_ref[0, rows, span], preferred_element_type=jnp.float32)
            gate, up = (g, u) if gate is None else (gate + g, up + u)
        hidden[:, span] = (gate / (1.0 + jnp.exp(-gate)) * up).astype(jnp.bfloat16)
        return carry

    lax.fori_loop(0, units // tile, make_hidden, 0)
    values = hidden[...]
    for out_ref, chosen in ((send_ref, sent), (keep_ref, kept)):
        for j, offset in enumerate(chosen):
            span = pl.ds(pl.multiple_of((me ^ offset) * cols, cols), cols)
            part = jnp.dot(values, down_ref[0, :, span], preferred_element_type=jnp.float32)
            out_ref[j] = part.astype(out_ref.dtype)


def add_kernel(*refs):
    total = refs[0][...].astype(jnp.float32)
    for ref in refs[1:-1]:
        total = total + ref[...].astype(jnp.float32)
    refs[-1][...] = total.astype(refs[-1].dtype)


def add(*arrays):
    out = jax.ShapeDtypeStruct(arrays[0].shape, arrays[0].dtype)
    return call(add_kernel, [out], arrays, limit=8, flops=arrays[0].size * len(arrays), name="add")[0]


def pairwise(tokens, norm_gain, expert_ids, gate_weights, w_gate, w_up, w_down):
    tok_count, cols = tokens.shape
    top_count = expert_ids.shape[1]
    expert_count, part_count = lax.axis_size("ep"), lax.axis_size("tp")
    capacity = 3 * tok_count * top_count // (2 * expert_count)
    units = w_gate.shape[2]
    ids, weights = expert_ids.T, gate_weights.T
    gain = norm_gain.reshape(part_count, 1, cols)
    offsets = list(range(expert_count))
    piece = jax.ShapeDtypeStruct((capacity, cols), jnp.bfloat16)
    chosen = call(
        functools.partial(select_kernel, offsets),
        [piece] * expert_count,
        (ids, tokens),
        flops=2 * expert_count * capacity * tok_count * cols,
        name="select",
    )
    bits = [1 << b for b in reversed(range(part_count.bit_length() - 1))]
    arrived = [chosen[0]] + [exchange(chosen[s], "ep", s) for s in offsets[1:]]
    results = []
    for s in offsets:
        parts, places = [arrived[s]], [0]
        for bit in bits:
            parts = parts + [exchange(p, "tp", bit) for p in parts]
            places = places + [p ^ bit for p in places]
        last = bits[-1]
        kept = [p for p in range(part_count) if not p & last]
        sent = [p ^ last for p in kept]
        half = jax.ShapeDtypeStruct((len(kept), capacity, cols), jnp.bfloat16)
        keep, send = call(
            functools.partial(expert_kernel, places, kept, sent),
            [half, half],
            (gain, w_gate, w_up, w_down, *parts),
            scratch=[
                pltpu.VMEM((part_count, capacity, cols), jnp.bfloat16),
                pltpu.VMEM((capacity, units), jnp.bfloat16),
            ],
            limit=24,
            flops=6 * capacity * cols * part_count * units,
            name="expert",
        )
        back = exchange(send, "tp", last)
        addends = {p: [keep[i], back[i]] for i, p in enumerate(kept)}
        for bit in reversed(bits[:-1]):
            leaving = [p for p in addends if p & bit]
            for p in leaving:
                addends[p ^ bit].append(exchange(add(*addends.pop(p)), "tp", bit))
        done = add(*addends[0])
        results.append(done if s == 0 else exchange(done, "ep", s))
    return call(
        functools.partial(combine_kernel, offsets),
        [jax.ShapeDtypeStruct(tokens.shape, tokens.dtype)],
        (ids, weights, *results),
        flops=4 * expert_count * capacity * tok_count * cols,
        name="combine",
    )[0]


def collective(tokens, norm_gain, expert_ids, gate_weights, w_gate, w_up, w_down):
    tok_count = tokens.shape[0]
    top_count = expert_ids.shape[1]
    expert_count = lax.axis_size("ep")
    capacity = 3 * tok_count * top_count // (2 * expert_count)
    model_width = norm_gain.shape[0]
    flat_ids = expert_ids.reshape(-1)
    onehot = (flat_ids[:, None] == jnp.arange(expert_count, dtype=jnp.int32)[None, :]).astype(
        jnp.int32
    )
    earlier = jnp.cumsum(onehot, axis=0) - onehot
    slot_index = jnp.sum(earlier * onehot, axis=1)
    dest_index = flat_ids * capacity + slot_index
    owner_index = jnp.arange(tok_count * top_count, dtype=jnp.int32) // top_count
    slot_token = (
        jnp.full((expert_count * capacity,), tok_count, jnp.int32).at[dest_index].set(owner_index)
    )
    tok_values = tokens.astype(jnp.float32)
    square_sum = lax.psum(jnp.sum(tok_values * tok_values, axis=1, keepdims=True), "tp")
    col_count = tokens.shape[1]
    gain_part = lax.dynamic_slice_in_dim(norm_gain, lax.axis_index("tp") * col_count, col_count)
    normed = (tok_values * lax.rsqrt(square_sum / model_width + epsilon) * gain_part).astype(
        jnp.bfloat16
    )
    buffer = jnp.take(normed, slot_token, axis=0, mode="fill", fill_value=0).reshape(
        expert_count, capacity, -1
    )
    received = lax.all_to_all(buffer, "ep", split_axis=0, concat_axis=0, tiled=True)
    source_count, item_count, col_count = received.shape
    tok_rows = received.reshape(-1, col_count)
    col_piece = lax.all_gather(tok_rows, "tp", axis=1, tiled=True)
    gate_part = jnp.dot(col_piece, w_gate[0], preferred_element_type=jnp.float32)
    up_part = jnp.dot(col_piece, w_up[0], preferred_element_type=jnp.float32)
    hidden = (jax.nn.silu(gate_part) * up_part).astype(jnp.bfloat16)
    partial_value = jnp.dot(hidden, w_down[0], preferred_element_type=jnp.float32)
    partial_value = partial_value.reshape(source_count, item_count, -1)
    summed = lax.psum_scatter(
        partial_value.astype(jnp.bfloat16), "tp", scatter_dimension=2, tiled=True
    )
    came_back = lax.all_to_all(summed, "ep", split_axis=0, concat_axis=0, tiled=True)
    picked = came_back.reshape(expert_count * capacity, -1)[dest_index].astype(jnp.float32)
    weighted = picked * gate_weights.reshape(-1)[:, None]
    return jnp.sum(weighted.reshape(tok_count, top_count, -1), axis=1).astype(jnp.bfloat16)


def solution(mesh):
    sizes = dict(mesh.shape)
    few = sizes["ep"] * sizes["tp"] <= 16
    plan = pairwise if few and is_power(sizes["ep"]) and is_power(sizes["tp"]) else collective
    return jax.shard_map(
        plan,
        mesh=mesh,
        in_specs=(
            P(("grp", "ep"), "tp"),
            P(),
            P(("grp", "ep"), None),
            P(("grp", "ep"), None),
            P("ep", None, "tp"),
            P("ep", None, "tp"),
            P("ep", "tp", None),
        ),
        out_specs=P(("grp", "ep"), "tp"),
        check_vma=False,
    )
```
